32 devices in a mesh: grp: 2 (over y), sp: 4 (over z), tp: 4 (over x, core).
Axes of the slice: x: 2, y: 2, z: 4, core: 2. Of those that a mesh axis runs over, the one named last changes fastest.
Arguments:
- tokens: bfloat16 [3072, 2048], P(('grp', 'sp')), parts along dimension 0, may hold values from -6 to 6
- norm_gain: float32 [2048], replicated, may hold values from 0.1 to 1.9
- w_query: bfloat16 [2048, 1024], P(None, 'tp'), may hold values from -0.088388348 to 0.088388348
- w_key: bfloat16 [2048, 1024], P(None, 'tp'), may hold values from -1.5467961 to 1.5467961
- w_value: bfloat16 [2048, 1024], P(None, 'tp'), may hold values from -0.30935922 to 0.30935922
- out_gain: float32 [1024], P('tp'), may hold values from 0.1 to 1.9
- w_out: bfloat16 [1024, 2048], P('tp'), may hold values from -0.1875 to 0.1875
Outputs:
- mixed: bfloat16 [3072, 2048], P(('grp', 'sp', 'tp')), parts along dimension 0
The draws below stay inside these ranges and needn't reach their ends.
There are 2 independent parts, one for each index of `grp`. The reference program is written for one: setup_inputs(seed, part) draws one part's arguments, and reference() takes and returns one part's arrays. A program takes and returns all parts, laid end to end along the dimension named above; an argument that names none is the same for every part. Nothing has to cross between parts.
All inputs are finite; a program needn't handle non-finite values.
Results may differ from the reference program's by a relative error of at most 0.015.
Values may be sent and summed in bfloat16 or wider, within the bound.
A program may use at most 64 MiB of HBM per device.

```python
from functools import reduce
import jax
import jax.numpy as jnp
from jax import lax

D = 2048
HEADS = 16
HEAD_DIM = 64
WINDOW_FIRST = 128
WINDOW_SECOND = 512
DILATION_SECOND = 4
WINDOW_THIRD = 2048
DILATION_THIRD = 16
SEQ = 1536
WIDTH = 1024
N_TP = 4


def query_raw(key):
    base = jax.random.fold_in(key, 11)
    raw = jnp.clip(jax.random.normal(base, (D, HEADS * HEAD_DIM), jnp.float32), -4.0, 4.0)
    return raw * D ** (-0.5)


def draw_w_query(key, part):
    return query_raw(key).astype(jnp.bfloat16)


def draw_w_key(key, part):
    noise = jnp.clip(jax.random.normal(jax.random.fold_in(key, 23), (D, HEADS * HEAD_DIM), jnp.float32), -4.0, 4.0) * D ** (-0.5)
    result = noise
    return result.astype(jnp.bfloat16)


def draw_w_value(key, part):
    base = jax.random.fold_in(key, 41)
    spread_key = jax.random.fold_in(key, 43)
    raw = jnp.clip(jax.random.normal(base, (D, HEADS * HEAD_DIM), jnp.float32), -4.0, 4.0)
    factors = jnp.exp(jax.random.uniform(spread_key, (HEADS,), jnp.float32, -1.2, 1.2))
    result = raw * D ** (-0.5) * jnp.repeat(factors, HEAD_DIM)[None, :]
    return result.astype(jnp.bfloat16)


def shard_levels(own_key, shape, pieces, low, high):
    gain = 1.0
    for position, shards_of in pieces:
        draws = jax.random.uniform(jax.random.fold_in(jax.random.fold_in(own_key, 6), position), (shards_of,), jnp.float32, low / len(pieces), high / len(pieces))
        gain = gain * jnp.repeat(jnp.exp(draws), shape[position] // shards_of).reshape((-1,) + (1,) * (len(shape) - 1 - position))
    return gain


def normal_values(own_key, dims, width, most, split=(), kind=jnp.bfloat16):
    entries = jax.random.normal(own_key, dims, jnp.float32) * width
    if len(split) > 0:
        entries = shard_levels(own_key, dims, split, -0.22, 0.18) * entries
    return jnp.clip(entries, min=-most, max=most).astype(kind)


def setup_inputs(seed: int = 0, part: int = 0) -> dict:
    key_of = jax.random.split(jax.random.key(seed), 8)
    part_keys = jax.random.split(jax.random.fold_in(key_of[7], part), 8)
    return {
        "tokens": normal_values(part_keys[0], (SEQ, D), 1.0, 6.0, ((0, 4),)),
        "norm_gain": jnp.clip(1.0 + 0.18 * jax.random.normal(key_of[1], (D,), jnp.float32), 0.1, 1.9),
        "w_query": draw_w_query(jax.random.fold_in(key_of[7], 71), part),
        "w_key": draw_w_key(jax.random.fold_in(key_of[7], 71), part),
        "w_value": draw_w_value(jax.random.fold_in(key_of[7], 71), part),
        "out_gain": jnp.clip(1.0 + 0.18 * jax.random.normal(key_of[5], (WIDTH,), jnp.float32), 0.1, 1.9),
        "w_out": normal_values(key_of[6], (WIDTH, D), WIDTH ** -0.5, 0.1875, ((0, 4),)),
    }


EPS = 1e-06
NEG = -1e+30

def band_part(queries, key_rows, value_rows, span_len, dilation_step, first_key):
    query_len, head_count, head_width = queries.shape
    class_len = query_len // dilation_step
    block_len = class_len if class_len <= 128 else 128
    blocks = class_len // block_len
    window_len = block_len + span_len
    query_blk = queries.reshape(blocks, block_len, dilation_step, head_count, head_width)
    key_cls = key_rows.reshape(class_len + span_len, dilation_step, head_count, head_width)
    value_cls = value_rows.reshape(class_len + span_len, dilation_step, head_count, head_width)
    picks = jnp.arange(blocks, dtype=jnp.int32)[:, None] * block_len + jnp.arange(window_len, dtype=jnp.int32)[None, :]
    key_blk = key_cls[picks]
    value_blk = value_cls[picks]
    scores = jnp.einsum('jqchx,jkchx->jchqk', query_blk.astype(jnp.float32), key_blk.astype(jnp.float32)) * HEAD_DIM ** (-0.5)
    lag_steps = span_len + jnp.arange(block_len, dtype=jnp.int32)[:, None] - jnp.arange(window_len, dtype=jnp.int32)[None, :]
    inside = (lag_steps >= 0) & (lag_steps <= span_len)
    key_pos = first_key + (jnp.arange(blocks, dtype=jnp.int32)[:, None, None] * block_len + jnp.arange(window_len, dtype=jnp.int32)[None, None, :]) * dilation_step + jnp.arange(dilation_step, dtype=jnp.int32)[None, :, None]
    usable = inside[None, None, None] & (key_pos >= 0)[:, :, None, None, :]
    scores = jnp.where(usable, scores, NEG)
    row_max = lax.optimization_barrier(jnp.max(scores, axis=-1))
    weights = jnp.exp(scores - row_max[..., None])
    row_sum = lax.optimization_barrier(jnp.sum(weights, axis=-1))
    rounded = lax.optimization_barrier(weights.astype(jnp.bfloat16))
    weighted = jnp.einsum('jchqk,jkchx->jqchx', rounded.astype(jnp.float32), value_blk.astype(jnp.float32))
    weighted = weighted.reshape(query_len, head_count, head_width)
    row_max = jnp.transpose(row_max, (0, 3, 1, 2)).reshape(query_len, head_count)
    row_sum = jnp.transpose(row_sum, (0, 3, 1, 2)).reshape(query_len, head_count)
    return (weighted, row_max, row_sum)

def mixture(pattern_out):
    peak_max = reduce(jnp.maximum, [result[1] for result in pattern_out])
    numerator = reduce(lambda left, right: left + right, [jnp.exp(result[1] - peak_max)[..., None] * result[0] for result in pattern_out])
    denominator = reduce(lambda left, right: left + right, [jnp.exp(result[1] - peak_max) * result[2] for result in pattern_out])
    return numerator / denominator[..., None]

def reference(tokens, norm_gain, w_query, w_key, w_value, out_gain, w_out):
    seq_len = tokens.shape[0]
    tokens_f = tokens.astype(jnp.float32)
    inverse = lax.rsqrt(lax.optimization_barrier(jnp.mean(tokens_f * tokens_f, axis=-1)) + EPS)
    scaled = (tokens_f * norm_gain).astype(jnp.bfloat16)

    def project(weight):
        return (jnp.dot(scaled, weight, preferred_element_type=jnp.float32) * inverse[:, None]).astype(jnp.bfloat16)

    def by_head(matrix):
        return jnp.moveaxis(matrix.reshape(seq_len, HEADS, HEAD_DIM), 1, 0)[:, :, None, :]
    queries = by_head(project(w_query))
    key_rows = by_head(project(w_key))
    value_rows = by_head(project(w_value))
    head_patterns = ((WINDOW_FIRST, 1), (WINDOW_SECOND, DILATION_SECOND), (WINDOW_THIRD, DILATION_THIRD))

    def head_attention(operands):
        head_q, head_k, head_v = operands
        results = []
        for window_span, dilation_step in head_patterns:
            padding = jnp.zeros((window_span, 1, HEAD_DIM), jnp.bfloat16)
            keys_ext = jnp.concatenate([padding, head_k], axis=0)
            values_ext = jnp.concatenate([padding, head_v], axis=0)
            results.append(band_part(head_q, keys_ext, values_ext, window_span // dilation_step, dilation_step, jnp.int32(-window_span)))
        return mixture(results)
    attended = lax.map(head_attention, (queries, key_rows, value_rows))
    attended = jnp.moveaxis(attended[:, :, 0, :], 0, 1).reshape(seq_len, WIDTH)
    out_scale = lax.rsqrt(lax.optimization_barrier(jnp.sum(attended * attended, axis=-1)) / WIDTH + EPS)
    gated = (attended * out_gain).astype(jnp.bfloat16)
    block_w = WIDTH // N_TP

    def add_block(accum, block_idx):
        start_col = (block_idx * block_w).astype(jnp.int32)
        product = jnp.dot(lax.dynamic_slice_in_dim(gated, start_col, block_w, 1), lax.dynamic_slice_in_dim(w_out, start_col, block_w, 0), preferred_element_type=jnp.float32)
        rounded = lax.optimization_barrier(product.astype(jnp.bfloat16))
        return (accum + rounded.astype(jnp.float32), None)
    summed, _ = lax.scan(add_block, jnp.zeros((seq_len, D), jnp.float32), jnp.arange(N_TP, dtype=jnp.int32))
    return (summed * out_scale[:, None]).astype(jnp.bfloat16)
```

```python
import functools
import math

import jax
import jax.numpy as jnp
from jax import lax
from jax.experimental import pallas as pl
from jax.experimental.pallas import tpu as pltpu
from jax.sharding import PartitionSpec as P

HEAD_DIM = 64
PATTERNS = ((128, 1), (512, 4), (2048, 16))
REACH = max(window for window, _ in PATTERNS)
EPS = 1e-06
NEG = -1e30
MESH = pl.DeviceIdType.MESH
ROW_BLOCK = 128
HALVES = 2


def log_multiplicity(rows, cols, first_lag):
    low, high = first_lag - (cols - 1), first_lag + rows - 1
    lag = (
        first_lag
        + lax.broadcasted_iota(jnp.int32, (rows, cols), 0)
        - lax.broadcasted_iota(jnp.int32, (rows, cols), 1)
    )
    count = jnp.zeros((rows, cols), jnp.int32)
    for window, dilation in PATTERNS:
        if high < 0 or low > window:
            continue
        reads = (lag & (dilation - 1)) == 0
        if low < 0:
            reads = reads & (lag >= 0)
        if high > window:
            reads = reads & (lag <= window)
        count = count + reads.astype(jnp.int32)
    return jnp.where(
        count == 0,
        NEG,
        jnp.where(count == 1, 0.0, jnp.where(count == 2, 1.0, math.log2(3.0))),
    )


def kernel(
    n_sp,
    n_tp,
    reach,
    tok_hbm,
    gain_ref,
    wq_hbm,
    wk_hbm,
    wv_hbm,
    og_hbm,
    wo_hbm,
    out_ref,
    tok,
    scaled,
    wq,
    wk,
    wv,
    og,
    wo,
    query,
    keys,
    values,
    top,
    total,
    partial,
    att,
    got,
    load_sem,
    k_send,
    k_recv,
    v_send,
    v_recv,
    wo_send,
    wo_recv,
    wo_fsend,
    og_send,
    og_recv,
    att_send,
    att_recv,
):
    z = lax.axis_index("sp")
    me = lax.axis_index("tp")
    rows, channels = query.shape
    heads = channels // HEAD_DIM
    share = rows // n_tp
    chips = n_tp // 2
    chip, core = me // 2, lax.rem(me, 2)
    sibling = chip * 2 + 1 - core
    has_next = z + 1 < n_sp

    loads = [
        pltpu.make_async_copy(source, target, load_sem.at[number])
        for number, (source, target) in enumerate(
            ((tok_hbm, tok), (wk_hbm, wk), (wv_hbm, wv), (wq_hbm, wq), (og_hbm, og.at[me]), (wo_hbm, wo.at[me]))
        )
    ]
    for load in loads:
        load.start()

    barrier = pltpu.get_barrier_semaphore()
    for step in range(1, n_tp):
        pl.semaphore_signal(
            barrier, inc=1, device_id={"tp": lax.rem(me + step, n_tp)}, device_id_type=MESH
        )

    @pl.when(z > 0)
    def _():
        pl.semaphore_signal(barrier, inc=1, device_id={"sp": z - 1}, device_id_type=MESH)

    @pl.when(has_next)
    def _():
        pl.semaphore_signal(barrier, inc=1, device_id={"sp": z + 1}, device_id_type=MESH)

    neighbours = (z > 0).astype(jnp.int32) + has_next.astype(jnp.int32)
    pl.semaphore_wait(barrier, n_tp - 1 + neighbours)

    half = channels // HALVES

    def part_of(piece):
        return pl.ds(piece * half, half)

    def wo_copy(slot, piece, target):
        return pltpu.make_async_remote_copy(
            src_ref=wo_hbm.at[part_of(piece)],
            dst_ref=wo.at[me, part_of(piece)],
            send_sem=wo_send.at[slot, piece],
            recv_sem=wo_recv.at[me, piece],
            device_id={"tp": target},
            device_id_type=MESH,
        )

    wo_targets = [lax.rem(chip + step, chips) * 2 + core for step in range(1, chips)] + [sibling]
    wo_sends = [
        wo_copy(slot, piece, target)
        for piece in range(HALVES)
        for slot, target in enumerate(wo_targets)
    ]
    for copy in wo_sends:
        copy.start()

    def wo_arrived(shard, piece):
        pltpu.make_async_remote_copy(
            src_ref=wo.at[shard, part_of(piece)],
            dst_ref=wo.at[shard, part_of(piece)],
            send_sem=wo_send.at[0, piece],
            recv_sem=wo_recv.at[shard, piece],
            device_id={"tp": sibling},
            device_id_type=MESH,
        ).wait_recv()

    def forward(step, piece):
        shard = lax.rem(chip + step, chips) * 2 + core
        return pltpu.make_async_remote_copy(
            src_ref=wo.at[shard, part_of(piece)],
            dst_ref=wo.at[shard, part_of(piece)],
            send_sem=wo_fsend.at[step, piece],
            recv_sem=wo_recv.at[shard, piece],
            device_id={"tp": sibling},
            device_id_type=MESH,
        )

    def forward_piece(piece):
        for step in range(1, chips):
            wo_arrived(lax.rem(chip + step, chips) * 2 + core, piece)
            forward(step, piece).start()

    og_sends = [
        pltpu.make_async_remote_copy(
            src_ref=og_hbm,
            dst_ref=og.at[me],
            send_sem=og_send.at[step],
            recv_sem=og_recv.at[me],
            device_id={"tp": lax.rem(me + step, n_tp)},
            device_id_type=MESH,
        )
        for step in range(1, n_tp)
    ]
    for copy in og_sends:
        copy.start()

    def relay(buffer, send, recv, distance):
        return pltpu.make_async_remote_copy(
            src_ref=buffer.at[distance],
            dst_ref=buffer.at[distance + 1],
            send_sem=send.at[distance],
            recv_sem=recv.at[distance + 1],
            device_id={"sp": z + 1},
            device_id_type=MESH,
        )

    def arrived(buffer, send, recv, distance):
        pltpu.make_async_remote_copy(
            src_ref=buffer.at[distance],
            dst_ref=buffer.at[distance],
            send_sem=send.at[0],
            recv_sem=recv.at[distance],
            device_id={"sp": z - 1},
            device_id_type=MESH,
        ).wait_recv()

    loads[0].wait()
    wide = tok[...].astype(jnp.float32)
    inverse = lax.rsqrt(jnp.mean(wide * wide, axis=-1, keepdims=True) + EPS)
    scaled[...] = (wide * gain_ref[...]).astype(jnp.bfloat16)

    def project(weight):
        product = jnp.dot(scaled[...], weight[...], preferred_element_type=jnp.float32)
        return (product * inverse).astype(jnp.bfloat16)

    loads[1].wait()
    keys[0] = project(wk)

    @pl.when(has_next)
    def _():
        relay(keys, k_send, k_recv, 0).start()

    loads[2].wait()
    values[0] = project(wv)

    @pl.when(has_next)
    def _():
        relay(values, v_send, v_recv, 0).start()

    loads[3].wait()
    query[...] = project(wq)

    lane_head = lax.broadcasted_iota(jnp.int32, (ROW_BLOCK, channels), 1) // HEAD_DIM
    factor = HEAD_DIM ** (-0.5) * math.log2(math.e)

    def attend(distance):
        for first in range(0, rows, ROW_BLOCK):
            cols = min(rows, first + ROW_BLOCK) if distance == 0 else rows
            first_lag = first + distance * rows
            if first_lag - (cols - 1) > REACH:
                continue
            block = pl.ds(first, ROW_BLOCK)
            bias = log_multiplicity(ROW_BLOCK, cols, first_lag)
            q_rows = query[block, :]
            key_rows = keys[distance, :cols, :]
            value_rows = values[distance, :cols, :]
            mixed, scale = None, None
            for head in range(heads):
                q_head = jnp.where(lane_head == head, q_rows, jnp.zeros_like(q_rows))
                scores = lax.dot_general(
                    q_head, key_rows, (((1,), (1,)), ((), ())), preferred_element_type=jnp.float32
                )
                scores = scores * factor + bias
                peak = jnp.max(scores, axis=-1, keepdims=True)
                if distance:
                    old = top[head, block, :]
                    peak = jnp.maximum(peak, old)
                    shrink = jnp.exp2(old - peak)
                weights = jnp.exp2(scores - peak)
                sums = jnp.sum(weights, axis=-1, keepdims=True)
                if distance:
                    sums = sums + shrink * total[head, block, :]
                    wide_shrink = jnp.broadcast_to(shrink, (ROW_BLOCK, channels))
                    scale = wide_shrink if scale is None else jnp.where(lane_head == head, wide_shrink, scale)
                top[head, block, :] = peak
                total[head, block, :] = sums
                product = jnp.dot(
                    weights.astype(jnp.bfloat16), value_rows, preferred_element_type=jnp.float32
                )
                mixed = product if mixed is None else jnp.where(lane_head == head, product, mixed)
            if distance:
                mixed = mixed + scale * partial[block, :]
            partial[block, :] = mixed

    attend(0)
    forwarded = 0
    for distance in range(1, reach + 1):

        @pl.when(z >= distance)
        def _():
            arrived(keys, k_send, k_recv, distance)
            if distance < reach:

                @pl.when(has_next)
                def _():
                    relay(keys, k_send, k_recv, distance).start()

            arrived(values, v_send, v_recv, distance)
            if distance < reach:

                @pl.when(has_next)
                def _():
                    relay(values, v_send, v_recv, distance).start()

            attend(distance)

        if forwarded < HALVES - 1 and distance >= 2:
            forward_piece(forwarded)
            forwarded += 1
    for piece in range(forwarded, HALVES):
        forward_piece(piece)

    def att_copy(step):
        target = lax.rem(me + step, n_tp)
        return pltpu.make_async_remote_copy(
            src_ref=att.at[target],
            dst_ref=got.at[me],
            send_sem=att_send.at[step],
            recv_sem=att_recv.at[me],
            device_id={"tp": target},
            device_id_type=MESH,
        )

    spread_head = lax.broadcasted_iota(jnp.int32, (share, channels), 1) // HEAD_DIM
    for part in range(n_tp):
        piece = pl.ds(part * share, share)
        denominator = jnp.broadcast_to(total[0, piece, :], (share, channels))
        for head in range(1, heads):
            denominator = jnp.where(
                spread_head == head,
                jnp.broadcast_to(total[head, piece, :], (share, channels)),
                denominator,
            )
        att[part] = (partial[piece, :] / denominator).astype(jnp.bfloat16)
    att_sends = [att_copy(step) for step in range(1, n_tp)]
    for copy in att_sends:
        copy.start()

    loads[4].wait()
    loads[5].wait()
    for step in range(1, n_tp):
        peer = lax.rem(me + step, n_tp)
        pltpu.make_async_remote_copy(
            src_ref=og_hbm,
            dst_ref=og.at[peer],
            send_sem=og_send.at[step],
            recv_sem=og_recv.at[peer],
            device_id={"tp": peer},
            device_id_type=MESH,
        ).wait_recv()
    for piece in range(HALVES):
        wo_arrived(sibling, piece)
        for step in range(1, chips):
            wo_arrived(lax.rem(chip + step, chips) * 2 + 1 - core, piece)

    def norm_and_gate(rows_of, gain_of):
        row_values = rows_of.astype(jnp.float32)
        return (
            jnp.sum(row_values * row_values, axis=-1, keepdims=True),
            (row_values * gain_of).astype(jnp.bfloat16),
        )

    squares, gated = norm_and_gate(att[me], og[me])
    summed = jnp.dot(gated, wo[me], preferred_element_type=jnp.float32)
    for step in range(1, n_tp):
        peer = lax.rem(me + step, n_tp)
        pltpu.make_async_remote_copy(
            src_ref=att.at[peer],
            dst_ref=got.at[peer],
            send_sem=att_send.at[step],
            recv_sem=att_recv.at[peer],
            device_id={"tp": peer},
            device_id_type=MESH,
        ).wait_recv()
        more, gated = norm_and_gate(got[peer], og[peer])
        squares = squares + more
        summed = summed + jnp.dot(gated, wo[peer], preferred_element_type=jnp.float32)
    norm = lax.rsqrt(squares / (channels * n_tp) + EPS)
    out_ref[...] = (summed * norm).astype(jnp.bfloat16)

    for copy in wo_sends + og_sends + att_sends:
        copy.wait_send()
    for piece in range(HALVES):
        for step in range(1, chips):
            forward(step, piece).wait_send()
    for distance in range(reach):

        @pl.when(has_next & (z >= distance))
        def _():
            relay(keys, k_send, k_recv, distance).wait_send()
            relay(values, v_send, v_recv, distance).wait_send()


def on_device(n_sp, n_tp, tokens, norm_gain, w_query, w_key, w_value, out_gain, w_out):
    rows, width = tokens.shape
    channels = w_query.shape[1]
    heads = channels // HEAD_DIM
    share = rows // n_tp
    reach = min(-(-REACH // rows), n_sp - 1)
    hbm = pl.BlockSpec(memory_space=pl.ANY)
    vmem = pl.BlockSpec(memory_space=pltpu.VMEM)
    dma = pltpu.SemaphoreType.DMA
    bf16, f32 = jnp.bfloat16, jnp.float32
    return pl.pallas_call(
        functools.partial(kernel, n_sp, n_tp, reach),
        out_shape=jax.ShapeDtypeStruct((share, w_out.shape[1]), bf16),
        in_specs=[hbm, vmem, hbm, hbm, hbm, hbm, hbm],
        out_specs=vmem,
        scratch_shapes=[
            pltpu.VMEM((rows, width), bf16),
            pltpu.VMEM((rows, width), bf16),
            pltpu.VMEM((width, channels), bf16),
            pltpu.VMEM((width, channels), bf16),
            pltpu.VMEM((width, channels), bf16),
            pltpu.VMEM((n_tp, 1, channels), f32),
            pltpu.VMEM((n_tp,) + w_out.shape, bf16),
            pltpu.VMEM((rows, channels), bf16),
            pltpu.VMEM((reach + 1, rows, channels), bf16),
            pltpu.VMEM((reach + 1, rows, channels), bf16),
            pltpu.VMEM((heads, rows, 1), f32),
            pltpu.VMEM((heads, rows, 1), f32),
            pltpu.VMEM((rows, channels), f32),
            pltpu.VMEM((n_tp, share, channels), bf16),
            pltpu.VMEM((n_tp, share, channels), bf16),
            dma((6,)),
            dma((reach + 1,)),
            dma((reach + 1,)),
            dma((reach + 1,)),
            dma((reach + 1,)),
            dma((n_tp // 2, HALVES)),
            dma((n_tp, HALVES)),
            dma((n_tp // 2, HALVES)),
            dma((n_tp,)),
            dma((n_tp,)),
            dma((n_tp,)),
            dma((n_tp,)),
        ],
        compiler_params=pltpu.CompilerParams(
            collective_id=0, has_side_effects=True, vmem_limit_bytes=60 * 1024 * 1024
        ),
    )(tokens, norm_gain[None, :], w_query, w_key, w_value, out_gain[None, :], w_out)


def solution(mesh):
    in_specs = (
        P(("grp", "sp"), None),
        P(),
        P(None, "tp"),
        P(None, "tp"),
        P(None, "tp"),
        P("tp"),
        P("tp", None),
    )
    out_specs = P(("grp", "sp", "tp"), None)
    return jax.shard_map(
        functools.partial(on_device, mesh.shape["sp"], mesh.shape["tp"]),
        mesh=mesh,
        in_specs=in_specs,
        out_specs=out_specs,
        check_vma=False,
    )
```

```python
import functools
import math

import jax
import jax.numpy as jnp
from jax import lax
from jax.experimental import pallas as pl
from jax.experimental.pallas import tpu as pltpu
from jax.sharding import PartitionSpec as P

HEAD_DIM = 64
PATTERNS = ((128, 1), (512, 4), (2048, 16))
REACH = max(window for window, _ in PATTERNS)
EPS = 1e-06
NEG = -1e30
MESH = pl.DeviceIdType.MESH
ROW_BLOCK = 128
PIECES = 4


def log_multiplicity(rows, cols, first_lag):
    low, high = first_lag - (cols - 1), first_lag + rows - 1
    lag = (
        first_lag
        + lax.broadcasted_iota(jnp.int32, (rows, cols), 0)
        - lax.broadcasted_iota(jnp.int32, (rows, cols), 1)
    )
    count = jnp.zeros((rows, cols), jnp.int32)
    for window, dilation in PATTERNS:
        if high < 0 or low > window:
            continue
        reads = (lag & (dilation - 1)) == 0
        if low < 0:
            reads = reads & (lag >= 0)
        if high > window:
            reads = reads & (lag <= window)
        count = count + reads.astype(jnp.int32)
    return jnp.where(
        count == 0,
        NEG,
        jnp.where(count == 1, 0.0, jnp.where(count == 2, 1.0, math.log2(3.0))),
    )


def kernel(
    n_grp,
    n_sp,
    n_tp,
    reach,
    tok_hbm,
    gain_ref,
    wq_hbm,
    wk_hbm,
    wv_hbm,
    og_hbm,
    wo_hbm,
    out_ref,
    tok,
    scaled,
    wq,
    wk,
    wv,
    og,
    wo,
    query,
    kv,
    guest,
    top,
    total,
    partial,
    help_att,
    help_lse,
    back_att,
    back_lse,
    att,
    got,
    load_sem,
    kv_send,
    kv_recv,
    q_send,
    q_recv,
    help_send,
    back_recv,
    wo_send,
    wo_recv,
    wo_fsend,
    wo_ysend,
    og_send,
    og_recv,
    att_send,
    att_recv,
):
    z = lax.axis_index("sp")
    me = lax.axis_index("tp")
    grp = lax.axis_index("grp")
    rows = query.shape[1]
    lanes = query.shape[2]
    channels = 2 * lanes
    heads = lanes // HEAD_DIM
    share = rows // n_tp
    chips = n_tp // 2
    chip, core = me // 2, lax.rem(me, 2)
    sibling = chip * 2 + 1 - core
    has_next = z + 1 < n_sp
    helped = n_sp == 4 and reach == 3
    paired = n_grp % 2 == 0
    far = grp + 1 - 2 * lax.rem(grp, 2) if paired else grp
    side = lax.rem(grp, 2) if paired else 0

    loads = [
        pltpu.make_async_copy(source, target, load_sem.at[number])
        for number, (source, target) in enumerate(
            ((tok_hbm, tok), (wk_hbm, wk), (wv_hbm, wv), (wq_hbm, wq), (og_hbm, og.at[me]), (wo_hbm, wo.at[me]))
        )
    ]
    for load in loads:
        load.start()

    barrier = pltpu.get_barrier_semaphore()
    for step in range(1, n_tp):
        pl.semaphore_signal(
            barrier, inc=1, device_id={"tp": lax.rem(me + step, n_tp)}, device_id_type=MESH
        )

    if paired:
        pl.semaphore_signal(barrier, inc=1, device_id={"grp": far}, device_id_type=MESH)
    for hop in ((1, 2) if helped else (1,)):
        if hop == 1:
            backward, onward = z > 0, has_next
        else:
            backward, onward = z == 3, z == 1

        @pl.when(backward)
        def _():
            pl.semaphore_signal(barrier, inc=1, device_id={"sp": z - hop}, device_id_type=MESH)

        @pl.when(onward)
        def _():
            pl.semaphore_signal(barrier, inc=1, device_id={"sp": z + hop}, device_id_type=MESH)

    neighbours = (z > 0).astype(jnp.int32) + has_next.astype(jnp.int32)
    if helped:
        neighbours = neighbours + (z == 3).astype(jnp.int32) + (z == 1).astype(jnp.int32)
    pl.semaphore_wait(barrier, n_tp - 1 + int(paired) + neighbours)

    half = channels // PIECES
    own_pieces = PIECES // 2 if paired else PIECES

    def part_of(piece):
        return pl.ds(pl.multiple_of(piece * half, half), half)

    def wo_copy(slot, piece, target):
        return pltpu.make_async_remote_copy(
            src_ref=wo_hbm.at[part_of(piece)],
            dst_ref=wo.at[me, part_of(piece)],
            send_sem=wo_send.at[slot, piece],
            recv_sem=wo_recv.at[me, piece],
            device_id={"tp": target},
            device_id_type=MESH,
        )

    mine = [side * own_pieces + number for number in range(own_pieces)]
    theirs = [(1 - side) * own_pieces + number for number in range(own_pieces)] if paired else []
    across = [lax.rem(chip + step, chips) * 2 + core for step in range(1, chips)]
    wo_sends = [
        wo_copy(slot, piece, target) for piece in mine for slot, target in enumerate(across)
    ] + [wo_copy(chips - 1, piece, sibling) for piece in range(PIECES)]
    for copy in wo_sends:
        copy.start()

    def passed_on(shard, piece, send_sem, device):
        return pltpu.make_async_remote_copy(
            src_ref=wo.at[shard, part_of(piece)],
            dst_ref=wo.at[shard, part_of(piece)],
            send_sem=send_sem,
            recv_sem=wo_recv.at[shard, piece],
            device_id=device,
            device_id_type=MESH,
        )

    def wo_arrived(shard, piece):
        passed_on(shard, piece, wo_send.at[0, piece], {"tp": sibling}).wait_recv()

    forwards = []

    def forward(pieces, over_y):
        for piece in pieces:
            for step in range(1, chips):
                shard = across[step - 1]
                wo_arrived(shard, piece)
                copies = [passed_on(shard, piece, wo_fsend.at[step, piece], {"tp": sibling})]
                if over_y:
                    copies.insert(0, passed_on(shard, piece, wo_ysend.at[step, piece], {"grp": far}))
                for copy in copies:
                    copy.start()
                forwards.extend(copies)

    og_sends = [
        pltpu.make_async_remote_copy(
            src_ref=og_hbm,
            dst_ref=og.at[me],
            send_sem=og_send.at[step],
            recv_sem=og_recv.at[me],
            device_id={"tp": lax.rem(me + step, n_tp)},
            device_id_type=MESH,
        )
        for step in range(1, n_tp)
    ]
    for copy in og_sends:
        copy.start()

    def relay(part, distance):
        return pltpu.make_async_remote_copy(
            src_ref=kv.at[part, distance],
            dst_ref=kv.at[part, distance + 1],
            send_sem=kv_send.at[part, distance],
            recv_sem=kv_recv.at[part, distance + 1],
            device_id={"sp": z + 1},
            device_id_type=MESH,
        )

    def arrived(part, distance):
        pltpu.make_async_remote_copy(
            src_ref=kv.at[part, distance],
            dst_ref=kv.at[part, distance],
            send_sem=kv_send.at[part, 0],
            recv_sem=kv_recv.at[part, distance],
            device_id={"sp": z - 1},
            device_id_type=MESH,
        ).wait_recv()

    def ship(part, slot, target):
        return pltpu.make_async_remote_copy(
            src_ref=query.at[part],
            dst_ref=guest.at[slot],
            send_sem=q_send.at[part],
            recv_sem=q_recv.at[slot],
            device_id={"sp": target},
            device_id_type=MESH,
        )

    def guest_arrived(slot):
        ship(0, slot, z + 1).wait_recv()

    def send_back(slot, part, target):
        return [
            pltpu.make_async_remote_copy(
                src_ref=mine_ref.at[slot],
                dst_ref=their_ref.at[part],
                send_sem=help_send.at[slot, number],
                recv_sem=back_recv.at[part, number],
                device_id={"sp": target},
                device_id_type=MESH,
            )
            for number, (mine_ref, their_ref) in enumerate(((help_att, back_att), (help_lse, back_lse)))
        ]

    loads[0].wait()
    wide = tok[...].astype(jnp.float32)
    inverse = lax.rsqrt(jnp.mean(wide * wide, axis=-1, keepdims=True) + EPS)
    scaled[...] = (wide * gain_ref[...]).astype(jnp.bfloat16)

    def project(weight):
        product = jnp.dot(scaled[...], weight[...], preferred_element_type=jnp.float32)
        return (product * inverse).astype(jnp.bfloat16)

    def by_half(product):
        return product[:, :lanes], product[:, lanes:]

    loads[1].wait()
    kv[0, 0, 0], kv[1, 0, 0] = by_half(project(wk))
    loads[2].wait()
    kv[0, 0, 1], kv[1, 0, 1] = by_half(project(wv))

    @pl.when(has_next)
    def _():
        relay(0, 0).start()

    @pl.when(has_next & (z != 1) if helped else has_next)
    def _():
        relay(1, 0).start()

    loads[3].wait()
    query[0], query[1] = by_half(project(wq))
    if helped:

        @pl.when(z == 2)
        def _():
            ship(1, 0, 1).start()

        @pl.when(z == 3)
        def _():
            ship(1, 1, 1).start()
            ship(0, 1, 2).start()

    lane_head = lax.broadcasted_iota(jnp.int32, (ROW_BLOCK, lanes), 1) // HEAD_DIM
    factor = HEAD_DIM ** (-0.5) * math.log2(math.e)

    def spread(columns):
        result = jnp.broadcast_to(columns[0], (ROW_BLOCK, lanes))
        for head in range(1, heads):
            result = jnp.where(
                lane_head == head, jnp.broadcast_to(columns[head], (ROW_BLOCK, lanes)), result
            )
        return result

    def attend(parts, state_of, queries_of, slot, distance, fresh):
        for first in range(0, rows, ROW_BLOCK):
            cols = min(rows, first + ROW_BLOCK) if distance == 0 else rows
            first_lag = first + distance * rows
            if first_lag - (cols - 1) > REACH:
                continue
            block = pl.ds(first, ROW_BLOCK)
            bias = log_multiplicity(ROW_BLOCK, cols, first_lag)
            for part in parts:
                state = state_of(part)
                q_rows = queries_of(part)[block, :]
                key_rows = kv[part, slot, 0, :cols, :]
                value_rows = kv[part, slot, 1, :cols, :]
                mixed, shrinks = None, []
                for head in range(heads):
                    q_head = jnp.where(lane_head == head, q_rows, jnp.zeros_like(q_rows))
                    scores = lax.dot_general(
                        q_head,
                        key_rows,
                        (((1,), (1,)), ((), ())),
                        preferred_element_type=jnp.float32,
                    )
                    scores = scores * factor + bias
                    peak = jnp.max(scores, axis=-1, keepdims=True)
                    if not fresh:
                        old = top[state, head, block, :]
                        peak = jnp.maximum(peak, old)
                        shrinks.append(jnp.exp2(old - peak))
                    weights = jnp.exp2(scores - peak)
                    sums = jnp.sum(weights, axis=-1, keepdims=True)
                    if not fresh:
                        sums = sums + shrinks[head] * total[state, head, block, :]
                    top[state, head, block, :] = peak
                    total[state, head, block, :] = sums
                    product = jnp.dot(
                        weights.astype(jnp.bfloat16), value_rows, preferred_element_type=jnp.float32
                    )
                    mixed = product if mixed is None else jnp.where(lane_head == head, product, mixed)
                if not fresh:
                    mixed = mixed + spread(shrinks) * partial[state, block, :]
                partial[state, block, :] = mixed

    def own(parts, distance):
        attend(parts, lambda part: part, lambda part: query.at[part], distance, distance, distance == 0)

    def help_out(part, guest_slot, slot, distance, fresh):
        attend(
            [part], lambda _: 2 + guest_slot, lambda _: guest.at[guest_slot], slot, distance, fresh
        )

    def give_back(guest_slot, part, target):
        state = 2 + guest_slot
        lane = lax.broadcasted_iota(jnp.int32, (ROW_BLOCK, 128), 1)
        pick = (
            lax.broadcasted_iota(jnp.int32, (8, 128), 0) == lax.broadcasted_iota(jnp.int32, (8, 128), 1)
        ).astype(jnp.float32)
        for first in range(0, rows, ROW_BLOCK):
            block = pl.ds(first, ROW_BLOCK)
            sums = [total[state, head, block, :] for head in range(heads)]
            help_att[guest_slot, block, :] = (partial[state, block, :] / spread(sums)).astype(jnp.bfloat16)
            logs = jnp.zeros((ROW_BLOCK, 128), jnp.float32)
            for head in range(heads):
                column = top[state, head, block, :] + jnp.log2(sums[head])
                logs = jnp.where(lane == head, jnp.broadcast_to(column, (ROW_BLOCK, 128)), logs)
            help_lse[guest_slot, :, block] = lax.dot_general(
                pick,
                logs,
                (((1,), (1,)), ((), ())),
                precision=lax.Precision.HIGHEST,
                preferred_element_type=jnp.float32,
            )
        for copy in send_back(guest_slot, part, target):
            copy.start()

    def take_back(part):
        for copy in send_back(0, part, z):
            copy.wait_recv()
        eye = (
            lax.broadcasted_iota(jnp.int32, (ROW_BLOCK, ROW_BLOCK), 0)
            == lax.broadcasted_iota(jnp.int32, (ROW_BLOCK, ROW_BLOCK), 1)
        ).astype(jnp.float32)
        for first in range(0, rows, ROW_BLOCK):
            block = pl.ds(first, ROW_BLOCK)
            logs = lax.dot_general(
                eye,
                back_lse[part, :, block],
                (((1,), (1,)), ((), ())),
                precision=lax.Precision.HIGHEST,
                preferred_element_type=jnp.float32,
            )
            before, after = [], []
            for head in range(heads):
                column, old = logs[:, head : head + 1], top[part, head, block, :]
                peak = jnp.maximum(column, old)
                before.append(jnp.exp2(old - peak))
                after.append(jnp.exp2(column - peak))
                total[part, head, block, :] = total[part, head, block, :] * before[head] + after[head]
            partial[part, block, :] = partial[part, block, :] * spread(before) + back_att[
                part, block, :
            ].astype(jnp.float32) * spread(after)

    both = (0, 1)
    if helped:

        @pl.when(z != 1)
        def _():
            own(both, 0)

        @pl.when(z == 1)
        def _():
            own(both, 0)
            arrived(0, 1)
            relay(0, 1).start()
            guest_arrived(1)
            help_out(1, 1, 0, 2, True)
            guest_arrived(0)
            help_out(1, 0, 0, 1, True)
            own([0], 1)

        forward(mine[:1], paired)

        @pl.when(z == 1)
        def _():
            arrived(1, 1)
            help_out(1, 1, 1, 3, False)
            give_back(1, 1, 3)
            help_out(1, 0, 1, 2, False)
            give_back(0, 1, 2)
            own([1], 1)

        @pl.when(z == 2)
        def _():
            arrived(0, 1)
            guest_arrived(1)
            help_out(0, 1, 1, 2, True)
            own([0], 1)

        forward(mine[1:], paired)

        @pl.when(z == 2)
        def _():
            arrived(0, 2)
            help_out(0, 1, 2, 3, False)
            give_back(1, 0, 3)
            own([0], 2)
            take_back(1)

        @pl.when(z == 3)
        def _():
            arrived(0, 1)
            own([0], 1)
            arrived(1, 1)
            own([1], 1)
            take_back(1)
            take_back(0)

    else:
        own(both, 0)
        for distance in range(1, reach + 1):

            @pl.when(z >= distance)
            def _():
                for part in both:
                    arrived(part, distance)
                    if distance < reach:

                        @pl.when(has_next)
                        def _():
                            relay(part, distance).start()

                own(both, distance)

        forward(mine, paired)

    def att_copy(step):
        target = lax.rem(me + step, n_tp)
        return pltpu.make_async_remote_copy(
            src_ref=att.at[target],
            dst_ref=got.at[me],
            send_sem=att_send.at[step],
            recv_sem=att_recv.at[me],
            device_id={"tp": target},
            device_id_type=MESH,
        )

    spread_head = lax.broadcasted_iota(jnp.int32, (share, lanes), 1) // HEAD_DIM
    for target in range(n_tp):
        piece = pl.ds(target * share, share)
        for part in both:
            denominator = jnp.broadcast_to(total[part, 0, piece, :], (share, lanes))
            for head in range(1, heads):
                denominator = jnp.where(
                    spread_head == head,
                    jnp.broadcast_to(total[part, head, piece, :], (share, lanes)),
                    denominator,
                )
            att[target, :, part * lanes : (part + 1) * lanes] = (
                partial[part, piece, :] / denominator
            ).astype(jnp.bfloat16)
    att_sends = [att_copy(step) for step in range(1, n_tp)]
    for copy in att_sends:
        copy.start()

    forward(theirs, False)
    loads[4].wait()
    loads[5].wait()
    for step in range(1, n_tp):
        peer = lax.rem(me + step, n_tp)
        pltpu.make_async_remote_copy(
            src_ref=og_hbm,
            dst_ref=og.at[peer],
            send_sem=og_send.at[step],
            recv_sem=og_recv.at[peer],
            device_id={"tp": peer},
            device_id_type=MESH,
        ).wait_recv()
    for piece in range(PIECES):
        wo_arrived(sibling, piece)
        for step in range(1, chips):
            wo_arrived(lax.rem(chip + step, chips) * 2 + 1 - core, piece)

    def norm_and_gate(rows_of, gain_of):
        row_values = rows_of.astype(jnp.float32)
        return (
            jnp.sum(row_values * row_values, axis=-1, keepdims=True),
            (row_values * gain_of).astype(jnp.bfloat16),
        )

    squares, gated = norm_and_gate(att[me], og[me])
    summed = jnp.dot(gated, wo[me], preferred_element_type=jnp.float32)
    for step in range(1, n_tp):
        peer = lax.rem(me + step, n_tp)
        pltpu.make_async_remote_copy(
            src_ref=att.at[peer],
            dst_ref=got.at[peer],
            send_sem=att_send.at[step],
            recv_sem=att_recv.at[peer],
            device_id={"tp": peer},
            device_id_type=MESH,
        ).wait_recv()
        more, gated = norm_and_gate(got[peer], og[peer])
        squares = squares + more
        summed = summed + jnp.dot(gated, wo[peer], preferred_element_type=jnp.float32)
    norm = lax.rsqrt(squares / (channels * n_tp) + EPS)
    out_ref[...] = (summed * norm).astype(jnp.bfloat16)

    for copy in wo_sends + og_sends + att_sends + forwards:
        copy.wait_send()
    if helped:

        @pl.when(z == 1)
        def _():
            relay(0, 0).wait_send()
            relay(0, 1).wait_send()
            for copy in send_back(1, 1, 3) + send_back(0, 1, 2):
                copy.wait_send()

        @pl.when((z == 0) | (z == 2))
        def _():
            relay(0, 0).wait_send()
            relay(1, 0).wait_send()

        @pl.when(z == 2)
        def _():
            ship(1, 0, 1).wait_send()
            for copy in send_back(1, 0, 3):
                copy.wait_send()

        @pl.when(z == 3)
        def _():
            ship(1, 1, 1).wait_send()
            ship(0, 1, 2).wait_send()

    else:
        for distance in range(reach):

            @pl.when(has_next & (z >= distance))
            def _():
                for part in both:
                    relay(part, distance).wait_send()


def on_device(n_grp, n_sp, n_tp, tokens, norm_gain, w_query, w_key, w_value, out_gain, w_out):
    rows, width = tokens.shape
    channels = w_query.shape[1]
    lanes = channels // 2
    heads = lanes // HEAD_DIM
    share = rows // n_tp
    reach = min(-(-REACH // rows), n_sp - 1)
    hbm = pl.BlockSpec(memory_space=pl.ANY)
    vmem = pl.BlockSpec(memory_space=pltpu.VMEM)
    dma = pltpu.SemaphoreType.DMA
    bf16, f32 = jnp.bfloat16, jnp.float32
    return pl.pallas_call(
        functools.partial(kernel, n_grp, n_sp, n_tp, reach),
        out_shape=jax.ShapeDtypeStruct((share, w_out.shape[1]), bf16),
        in_specs=[hbm, vmem, hbm, hbm, hbm, hbm, hbm],
        out_specs=vmem,
        scratch_shapes=[
            pltpu.VMEM((rows, width), bf16),
            pltpu.VMEM((rows, width), bf16),
            pltpu.VMEM((width, channels), bf16),
            pltpu.VMEM((width, channels), bf16),
            pltpu.VMEM((width, channels), bf16),
            pltpu.VMEM((n_tp, 1, channels), f32),
            pltpu.VMEM((n_tp,) + w_out.shape, bf16),
            pltpu.VMEM((2, rows, lanes), bf16),
            pltpu.VMEM((2, reach + 1, 2, rows, lanes), bf16),
            pltpu.VMEM((2, rows, lanes), bf16),
            pltpu.VMEM((4, heads, rows, 1), f32),
            pltpu.VMEM((4, heads, rows, 1), f32),
            pltpu.VMEM((4, rows, lanes), f32),
            pltpu.VMEM((2, rows, lanes), bf16),
            pltpu.VMEM((2, 8, rows), f32),
            pltpu.VMEM((2, rows, lanes), bf16),
            pltpu.VMEM((2, 8, rows), f32),
            pltpu.VMEM((n_tp, share, channels), bf16),
            pltpu.VMEM((n_tp, share, channels), bf16),
            dma((6,)),
            dma((2, reach + 1)),
            dma((2, reach + 1)),
            dma((2,)),
            dma((2,)),
            dma((2, 2)),
            dma((2, 2)),
            dma((n_tp // 2, PIECES)),
            dma((n_tp, PIECES)),
            dma((n_tp // 2, PIECES)),
            dma((n_tp // 2, PIECES)),
            dma((n_tp,)),
            dma((n_tp,)),
            dma((n_tp,)),
            dma((n_tp,)),
        ],
        compiler_params=pltpu.CompilerParams(
            collective_id=0, has_side_effects=True, vmem_limit_bytes=60 * 1024 * 1024
        ),
    )(tokens, norm_gain[None, :], w_query, w_key, w_value, out_gain[None, :], w_out)


def solution(mesh):
    in_specs = (
        P(("grp", "sp"), None),
        P(),
        P(None, "tp"),
        P(None, "tp"),
        P(None, "tp"),
        P("tp"),
        P("tp", None),
    )
    out_specs = P(("grp", "sp", "tp"), None)
    return jax.shard_map(
        functools.partial(on_device, mesh.shape["grp"], mesh.shape["sp"], mesh.shape["tp"]),
        mesh=mesh,
        in_specs=in_specs,
        out_specs=out_specs,
        check_vma=False,
    )
```

```python
import functools
import math

import jax
import jax.numpy as jnp
from jax import lax
from jax.experimental import pallas as pl
from jax.experimental.pallas import tpu as pltpu
from jax.sharding import PartitionSpec as P

HEAD_DIM = 64
PATTERNS = ((128, 1), (512, 4), (2048, 16))
REACH = max(window for window, _ in PATTERNS)
EPS = 1e-06
NEG = -1e30
MESH = pl.DeviceIdType.MESH
ROW_BLOCK = 128
PIECES = 4


def log_multiplicity(rows, cols, first_lag):
    low, high = first_lag - (cols - 1), first_lag + rows - 1
    lag = (
        first_lag
        + lax.broadcasted_iota(jnp.int32, (rows, cols), 0)
        - lax.broadcasted_iota(jnp.int32, (rows, cols), 1)
    )
    count = jnp.zeros((rows, cols), jnp.int32)
    for window, dilation in PATTERNS:
        if high < 0 or low > window:
            continue
        reads = (lag & (dilation - 1)) == 0
        if low < 0:
            reads = reads & (lag >= 0)
        if high > window:
            reads = reads & (lag <= window)
        count = count + reads.astype(jnp.int32)
    return jnp.where(
        count == 0,
        NEG,
        jnp.where(count == 1, 0.0, jnp.where(count == 2, 1.0, math.log2(3.0))),
    )


def kernel(
    n_grp,
    n_sp,
    n_tp,
    reach,
    tok_hbm,
    gain_ref,
    wq_hbm,
    wk_hbm,
    wv_hbm,
    og_hbm,
    wo_hbm,
    out_ref,
    tok,
    scaled,
    wq,
    wk,
    wv,
    og,
    wo,
    query,
    kv,
    guest,
    allowed,
    top,
    total,
    partial,
    help_att,
    help_lse,
    back_att,
    back_lse,
    att,
    got,
    load_sem,
    kv_send,
    kv_recv,
    q_send,
    q_recv,
    help_send,
    back_recv,
    wo_send,
    wo_recv,
    wo_fsend,
    wo_ysend,
    og_send,
    og_recv,
    att_send,
    att_recv,
):
    z = lax.axis_index("sp")
    me = lax.axis_index("tp")
    grp = lax.axis_index("grp")
    rows = query.shape[1]
    lanes = query.shape[2]
    channels = 2 * lanes
    heads = lanes // HEAD_DIM
    share = rows // n_tp
    chips = n_tp // 2
    chip, core = me // 2, lax.rem(me, 2)
    sibling = chip * 2 + 1 - core
    has_next = z + 1 < n_sp
    helped = n_sp == 4 and reach == 3
    paired = n_grp % 2 == 0
    far = grp + 1 - 2 * lax.rem(grp, 2) if paired else grp
    side = lax.rem(grp, 2) if paired else 0

    loads = [
        pltpu.make_async_copy(source, target, load_sem.at[number])
        for number, (source, target) in enumerate(
            ((tok_hbm, tok), (wk_hbm, wk), (wv_hbm, wv), (wq_hbm, wq), (og_hbm, og.at[me]), (wo_hbm, wo.at[me]))
        )
    ]
    for load in loads:
        load.start()

    barrier = pltpu.get_barrier_semaphore()
    for step in range(1, n_tp):
        pl.semaphore_signal(
            barrier, inc=1, device_id={"tp": lax.rem(me + step, n_tp)}, device_id_type=MESH
        )

    if paired:
        pl.semaphore_signal(barrier, inc=1, device_id={"grp": far}, device_id_type=MESH)
    for hop in ((1, 2) if helped else (1,)):
        if hop == 1:
            backward, onward = z > 0, has_next
        else:
            backward, onward = z == 3, z == 1

        @pl.when(backward)
        def _():
            pl.semaphore_signal(barrier, inc=1, device_id={"sp": z - hop}, device_id_type=MESH)

        @pl.when(onward)
        def _():
            pl.semaphore_signal(barrier, inc=1, device_id={"sp": z + hop}, device_id_type=MESH)

    def mark(distances):
        for distance in distances:
            for first in range(0, rows, ROW_BLOCK):
                allowed[distance, pl.ds(first, ROW_BLOCK), :] = log_multiplicity(
                    ROW_BLOCK, rows, first + distance * rows
                )

    mark(range(1))
    neighbours = (z > 0).astype(jnp.int32) + has_next.astype(jnp.int32)
    if helped:
        neighbours = neighbours + (z == 3).astype(jnp.int32) + (z == 1).astype(jnp.int32)
    pl.semaphore_wait(barrier, n_tp - 1 + int(paired) + neighbours)

    half = channels // PIECES
    own_pieces = PIECES // 2 if paired else PIECES

    def part_of(piece):
        return pl.ds(pl.multiple_of(piece * half, half), half)

    def wo_copy(slot, piece, target):
        return pltpu.make_async_remote_copy(
            src_ref=wo_hbm.at[part_of(piece)],
            dst_ref=wo.at[me, part_of(piece)],
            send_sem=wo_send.at[slot, piece],
            recv_sem=wo_recv.at[me, piece],
            device_id={"tp": target},
            device_id_type=MESH,
        )

    mine = [side * own_pieces + number for number in range(own_pieces)]
    theirs = [(1 - side) * own_pieces + number for number in range(own_pieces)] if paired else []
    across = [lax.rem(chip + step, chips) * 2 + core for step in range(1, chips)]
    wo_sends = [
        wo_copy(slot, piece, target) for piece in mine for slot, target in enumerate(across)
    ] + [wo_copy(chips - 1, piece, sibling) for piece in range(PIECES)]
    for copy in wo_sends:
        copy.start()

    def passed_on(shard, piece, send_sem, device):
        return pltpu.make_async_remote_copy(
            src_ref=wo.at[shard, part_of(piece)],
            dst_ref=wo.at[shard, part_of(piece)],
            send_sem=send_sem,
            recv_sem=wo_recv.at[shard, piece],
            device_id=device,
            device_id_type=MESH,
        )

    def wo_arrived(shard, piece):
        passed_on(shard, piece, wo_send.at[0, piece], {"tp": sibling}).wait_recv()

    forwards = []

    def forward(pieces, over_y):
        for piece in pieces:
            for step in range(1, chips):
                shard = across[step - 1]
                wo_arrived(shard, piece)
                copies = [passed_on(shard, piece, wo_fsend.at[step, piece], {"tp": sibling})]
                if over_y:
                    copies.insert(0, passed_on(shard, piece, wo_ysend.at[step, piece], {"grp": far}))
                for copy in copies:
                    copy.start()
                forwards.extend(copies)

    og_sends = [
        pltpu.make_async_remote_copy(
            src_ref=og_hbm,
            dst_ref=og.at[me],
            send_sem=og_send.at[step],
            recv_sem=og_recv.at[me],
            device_id={"tp": lax.rem(me + step, n_tp)},
            device_id_type=MESH,
        )
        for step in range(1, n_tp)
    ]
    for copy in og_sends:
        copy.start()

    def relay(part, distance):
        return pltpu.make_async_remote_copy(
            src_ref=kv.at[part, distance],
            dst_ref=kv.at[part, distance + 1],
            send_sem=kv_send.at[part, distance],
            recv_sem=kv_recv.at[part, distance + 1],
            device_id={"sp": z + 1},
            device_id_type=MESH,
        )

    def arrived(part, distance):
        pltpu.make_async_remote_copy(
            src_ref=kv.at[part, distance],
            dst_ref=kv.at[part, distance],
            send_sem=kv_send.at[part, 0],
            recv_sem=kv_recv.at[part, distance],
            device_id={"sp": z - 1},
            device_id_type=MESH,
        ).wait_recv()

    def ship(part, slot, target):
        return pltpu.make_async_remote_copy(
            src_ref=query.at[part],
            dst_ref=guest.at[slot],
            send_sem=q_send.at[part],
            recv_sem=q_recv.at[slot],
            device_id={"sp": target},
            device_id_type=MESH,
        )

    def guest_arrived(slot):
        ship(0, slot, z + 1).wait_recv()

    def send_back(slot, part, target):
        return [
            pltpu.make_async_remote_copy(
                src_ref=mine_ref.at[slot],
                dst_ref=their_ref.at[part],
                send_sem=help_send.at[slot, number],
                recv_sem=back_recv.at[part, number],
                device_id={"sp": target},
                device_id_type=MESH,
            )
            for number, (mine_ref, their_ref) in enumerate(((help_att, back_att), (help_lse, back_lse)))
        ]

    loads[0].wait()
    wide = tok[...].astype(jnp.float32)
    inverse = lax.rsqrt(jnp.mean(wide * wide, axis=-1, keepdims=True) + EPS)
    scaled[...] = (wide * gain_ref[...]).astype(jnp.bfloat16)

    def project(weight):
        product = jnp.dot(scaled[...], weight[...], preferred_element_type=jnp.float32)
        return (product * inverse).astype(jnp.bfloat16)

    def by_half(product):
        return product[:, :lanes], product[:, lanes:]

    loads[1].wait()
    kv[0, 0, 0], kv[1, 0, 0] = by_half(project(wk))
    loads[2].wait()
    kv[0, 0, 1], kv[1, 0, 1] = by_half(project(wv))

    @pl.when(has_next)
    def _():
        relay(0, 0).start()

    @pl.when(has_next & (z != 1) if helped else has_next)
    def _():
        relay(1, 0).start()

    loads[3].wait()
    query[0], query[1] = by_half(project(wq))
    if helped:

        @pl.when(z == 2)
        def _():
            ship(1, 0, 1).start()

        @pl.when(z == 3)
        def _():
            ship(1, 1, 1).start()
            ship(0, 1, 2).start()

    mark(range(1, reach + 1))
    lane_head = lax.broadcasted_iota(jnp.int32, (ROW_BLOCK, lanes), 1) // HEAD_DIM
    factor = HEAD_DIM ** (-0.5) * math.log2(math.e)

    def spread(columns):
        result = jnp.broadcast_to(columns[0], (ROW_BLOCK, lanes))
        for head in range(1, heads):
            result = jnp.where(
                lane_head == head, jnp.broadcast_to(columns[head], (ROW_BLOCK, lanes)), result
            )
        return result

    def stacked(rows_of):
        return jnp.concatenate(
            [jnp.where(lane_head == head, rows_of, jnp.zeros_like(rows_of)) for head in range(heads)],
            axis=0,
        )

    ones = jnp.ones((rows, lanes), jnp.bfloat16)

    def by_head(tall):
        result = tall[:ROW_BLOCK]
        for head in range(1, heads):
            result = jnp.where(
                lane_head == head, tall[head * ROW_BLOCK : (head + 1) * ROW_BLOCK], result
            )
        return result

    def attend(parts, state_of, queries_of, slot, distance, fresh):
        for part in parts:
            state = state_of(part)
            for first in range(0, rows, ROW_BLOCK):
                cols = min(rows, first + ROW_BLOCK) if distance == 0 else rows
                if first + distance * rows - (cols - 1) > REACH:
                    continue
                block = pl.ds(first, ROW_BLOCK)
                scores = lax.dot_general(
                    stacked(queries_of(part)[block, :]),
                    kv[part, slot, 0, :cols, :],
                    (((1,), (1,)), ((), ())),
                    preferred_element_type=jnp.float32,
                )
                bias = allowed[distance, block, :cols]
                scores = scores * factor + jnp.concatenate([bias] * heads, axis=0)
                peak = jnp.max(scores, axis=-1, keepdims=True)
                if not fresh:
                    old = jnp.concatenate([top[state, head, block, :] for head in range(heads)], axis=0)
                    peak = jnp.maximum(peak, old)
                    shrink = by_head(jnp.broadcast_to(jnp.exp2(old - peak), (heads * ROW_BLOCK, lanes)))
                for head in range(heads):
                    top[state, head, block, :] = peak[head * ROW_BLOCK : (head + 1) * ROW_BLOCK]
                weights = jnp.exp2(scores - peak).astype(jnp.bfloat16)
                extended = jnp.concatenate([kv[part, slot, 1, :cols, :], ones[:cols]], axis=1)
                product = jnp.dot(weights, extended, preferred_element_type=jnp.float32)
                mixed, sums = by_head(product[:, :lanes]), by_head(product[:, lanes:])
                if not fresh:
                    mixed = mixed + shrink * partial[state, block, :]
                    sums = sums + shrink * total[state, block, :]
                partial[state, block, :] = mixed
                total[state, block, :] = sums

    def own(parts, distance):
        attend(parts, lambda part: part, lambda part: query.at[part], distance, distance, distance == 0)

    def help_out(part, guest_slot, slot, distance, fresh):
        attend(
            [part], lambda _: 2 + guest_slot, lambda _: guest.at[guest_slot], slot, distance, fresh
        )

    def give_back(guest_slot, part, target):
        state = 2 + guest_slot
        lane = lax.broadcasted_iota(jnp.int32, (ROW_BLOCK, 128), 1)
        pick = (
            lax.broadcasted_iota(jnp.int32, (8, 128), 0) == lax.broadcasted_iota(jnp.int32, (8, 128), 1)
        ).astype(jnp.float32)
        for first in range(0, rows, ROW_BLOCK):
            block = pl.ds(first, ROW_BLOCK)
            sums = total[state, block, :]
            help_att[guest_slot, block, :] = (partial[state, block, :] / sums).astype(jnp.bfloat16)
            logs = jnp.zeros((ROW_BLOCK, 128), jnp.float32)
            for head in range(heads):
                column = top[state, head, block, :] + jnp.log2(sums[:, head * HEAD_DIM : head * HEAD_DIM + 1])
                logs = jnp.where(lane == head, jnp.broadcast_to(column, (ROW_BLOCK, 128)), logs)
            help_lse[guest_slot, :, block] = lax.dot_general(
                pick,
                logs,
                (((1,), (1,)), ((), ())),
                precision=lax.Precision.HIGHEST,
                preferred_element_type=jnp.float32,
            )
        for copy in send_back(guest_slot, part, target):
            copy.start()

    def take_back(part):
        for copy in send_back(0, part, z):
            copy.wait_recv()
        eye = (
            lax.broadcasted_iota(jnp.int32, (ROW_BLOCK, ROW_BLOCK), 0)
            == lax.broadcasted_iota(jnp.int32, (ROW_BLOCK, ROW_BLOCK), 1)
        ).astype(jnp.float32)
        for first in range(0, rows, ROW_BLOCK):
            block = pl.ds(first, ROW_BLOCK)
            logs = lax.dot_general(
                eye,
                back_lse[part, :, block],
                (((1,), (1,)), ((), ())),
                precision=lax.Precision.HIGHEST,
                preferred_element_type=jnp.float32,
            )
            before, after = [], []
            for head in range(heads):
                column, old = logs[:, head : head + 1], top[part, head, block, :]
                peak = jnp.maximum(column, old)
                before.append(jnp.exp2(old - peak))
                after.append(jnp.exp2(column - peak))
            wide_before, wide_after = spread(before), spread(after)
            total[part, block, :] = total[part, block, :] * wide_before + wide_after
            partial[part, block, :] = (
                partial[part, block, :] * wide_before
                + back_att[part, block, :].astype(jnp.float32) * wide_after
            )

    both = (0, 1)
    if helped:

        @pl.when(z != 1)
        def _():
            own(both, 0)

        @pl.when(z == 1)
        def _():
            own(both, 0)
            arrived(0, 1)
            relay(0, 1).start()
            guest_arrived(1)
            help_out(1, 1, 0, 2, True)
            guest_arrived(0)
            help_out(1, 0, 0, 1, True)
            own([0], 1)

        forward(mine[:1], paired)

        @pl.when(z == 1)
        def _():
            arrived(1, 1)
            help_out(1, 1, 1, 3, False)
            give_back(1, 1, 3)
            help_out(1, 0, 1, 2, False)
            give_back(0, 1, 2)
            own([1], 1)

        @pl.when(z == 2)
        def _():
            arrived(0, 1)
            guest_arrived(1)
            help_out(0, 1, 1, 2, True)
            own([0], 1)

        forward(mine[1:], paired)

        @pl.when(z == 2)
        def _():
            arrived(0, 2)
            help_out(0, 1, 2, 3, False)
            give_back(1, 0, 3)
            own([0], 2)
            take_back(1)

        @pl.when(z == 3)
        def _():
            arrived(0, 1)
            own([0], 1)
            arrived(1, 1)
            own([1], 1)
            take_back(1)
            take_back(0)

    else:
        own(both, 0)
        for distance in range(1, reach + 1):

            @pl.when(z >= distance)
            def _():
                for part in both:
                    arrived(part, distance)
                    if distance < reach:

                        @pl.when(has_next)
                        def _():
                            relay(part, distance).start()

                own(both, distance)

        forward(mine, paired)

    def att_copy(step):
        target = lax.rem(me + step, n_tp)
        return pltpu.make_async_remote_copy(
            src_ref=att.at[target],
            dst_ref=got.at[me],
            send_sem=att_send.at[step],
            recv_sem=att_recv.at[me],
            device_id={"tp": target},
            device_id_type=MESH,
        )

    for target in range(n_tp):
        piece = pl.ds(target * share, share)
        for part in both:
            att[target, :, part * lanes : (part + 1) * lanes] = (
                partial[part, piece, :] / total[part, piece, :]
            ).astype(jnp.bfloat16)
    att_sends = [att_copy(step) for step in range(1, n_tp)]
    for copy in att_sends:
        copy.start()

    forward(theirs, False)
    loads[4].wait()
    loads[5].wait()
    for step in range(1, n_tp):
        peer = lax.rem(me + step, n_tp)
        pltpu.make_async_remote_copy(
            src_ref=og_hbm,
            dst_ref=og.at[peer],
            send_sem=og_send.at[step],
            recv_sem=og_recv.at[peer],
            device_id={"tp": peer},
            device_id_type=MESH,
        ).wait_recv()
    for piece in range(PIECES):
        wo_arrived(sibling, piece)
        for step in range(1, chips):
            wo_arrived(lax.rem(chip + step, chips) * 2 + 1 - core, piece)

    def norm_and_gate(rows_of, gain_of):
        row_values = rows_of.astype(jnp.float32)
        return (
            jnp.sum(row_values * row_values, axis=-1, keepdims=True),
            (row_values * gain_of).astype(jnp.bfloat16),
        )

    squares, gated = norm_and_gate(att[me], og[me])
    summed = jnp.dot(gated, wo[me], preferred_element_type=jnp.float32)
    for step in range(1, n_tp):
        peer = lax.rem(me + step, n_tp)
        pltpu.make_async_remote_copy(
            src_ref=att.at[peer],
            dst_ref=got.at[peer],
            send_sem=att_send.at[step],
            recv_sem=att_recv.at[peer],
            device_id={"tp": peer},
            device_id_type=MESH,
        ).wait_recv()
        more, gated = norm_and_gate(got[peer], og[peer])
        squares = squares + more
        summed = summed + jnp.dot(gated, wo[peer], preferred_element_type=jnp.float32)
    norm = lax.rsqrt(squares / (channels * n_tp) + EPS)
    out_ref[...] = (summed * norm).astype(jnp.bfloat16)

    for copy in wo_sends + og_sends + att_sends + forwards:
        copy.wait_send()
    if helped:

        @pl.when(z == 1)
        def _():
            relay(0, 0).wait_send()
            relay(0, 1).wait_send()
            for copy in send_back(1, 1, 3) + send_back(0, 1, 2):
                copy.wait_send()

        @pl.when((z == 0) | (z == 2))
        def _():
            relay(0, 0).wait_send()
            relay(1, 0).wait_send()

        @pl.when(z == 2)
        def _():
            ship(1, 0, 1).wait_send()
            for copy in send_back(1, 0, 3):
                copy.wait_send()

        @pl.when(z == 3)
        def _():
            ship(1, 1, 1).wait_send()
            ship(0, 1, 2).wait_send()

    else:
        for distance in range(reach):

            @pl.when(has_next & (z >= distance))
            def _():
                for part in both:
                    relay(part, distance).wait_send()


def on_device(n_grp, n_sp, n_tp, tokens, norm_gain, w_query, w_key, w_value, out_gain, w_out):
    rows, width = tokens.shape
    channels = w_query.shape[1]
    lanes = channels // 2
    heads = lanes // HEAD_DIM
    share = rows // n_tp
    reach = min(-(-REACH // rows), n_sp - 1)
    hbm = pl.BlockSpec(memory_space=pl.ANY)
    vmem = pl.BlockSpec(memory_space=pltpu.VMEM)
    dma = pltpu.SemaphoreType.DMA
    bf16, f32 = jnp.bfloat16, jnp.float32
    return pl.pallas_call(
        functools.partial(kernel, n_grp, n_sp, n_tp, reach),
        out_shape=jax.ShapeDtypeStruct((share, w_out.shape[1]), bf16),
        in_specs=[hbm, vmem, hbm, hbm, hbm, hbm, hbm],
        out_specs=vmem,
        scratch_shapes=[
            pltpu.VMEM((rows, width), bf16),
            pltpu.VMEM((rows, width), bf16),
            pltpu.VMEM((width, channels), bf16),
            pltpu.VMEM((width, channels), bf16),
            pltpu.VMEM((width, channels), bf16),
            pltpu.VMEM((n_tp, 1, channels), f32),
            pltpu.VMEM((n_tp,) + w_out.shape, bf16),
            pltpu.VMEM((2, rows, lanes), bf16),
            pltpu.VMEM((2, reach + 1, 2, rows, lanes), bf16),
            pltpu.VMEM((2, rows, lanes), bf16),
            pltpu.VMEM((reach + 1, rows, rows), f32),
            pltpu.VMEM((4, heads, rows, 1), f32),
            pltpu.VMEM((4, rows, lanes), f32),
            pltpu.VMEM((4, rows, lanes), f32),
            pltpu.VMEM((2, rows, lanes), bf16),
            pltpu.VMEM((2, 8, rows), f32),
            pltpu.VMEM((2, rows, lanes), bf16),
            pltpu.VMEM((2, 8, rows), f32),
            pltpu.VMEM((n_tp, share, channels), bf16),
            pltpu.VMEM((n_tp, share, channels), bf16),
            dma((6,)),
            dma((2, reach + 1)),
            dma((2, reach + 1)),
            dma((2,)),
            dma((2,)),
            dma((2, 2)),
            dma((2, 2)),
            dma((n_tp // 2, PIECES)),
            dma((n_tp, PIECES)),
            dma((n_tp // 2, PIECES)),
            dma((n_tp // 2, PIECES)),
            dma((n_tp,)),
            dma((n_tp,)),
            dma((n_tp,)),
            dma((n_tp,)),
        ],
        compiler_params=pltpu.CompilerParams(
            collective_id=0, has_side_effects=True, vmem_limit_bytes=60 * 1024 * 1024
        ),
    )(tokens, norm_gain[None, :], w_query, w_key, w_value, out_gain[None, :], w_out)


def solution(mesh):
    in_specs = (
        P(("grp", "sp"), None),
        P(),
        P(None, "tp"),
        P(None, "tp"),
        P(None, "tp"),
        P("tp"),
        P("tp", None),
    )
    out_specs = P(("grp", "sp", "tp"), None)
    return jax.shard_map(
        functools.partial(on_device, mesh.shape["grp"], mesh.shape["sp"], mesh.shape["tp"]),
        mesh=mesh,
        in_specs=in_specs,
        out_specs=out_specs,
        check_vma=False,
    )
```

```python
import functools
import math

import jax
import jax.numpy as jnp
from jax import lax
from jax.experimental import pallas as pl
from jax.experimental.pallas import tpu as pltpu
from jax.sharding import PartitionSpec as P

HEAD_DIM = 64
PATTERNS = ((128, 1), (512, 4), (2048, 16))
REACH = max(window for window, _ in PATTERNS)
EPS = 1e-06
NEG = -1e30
MESH = pl.DeviceIdType.MESH
ROW_BLOCK = 128
PIECES = 8


def log_multiplicity(rows, cols, first_lag):
    low, high = first_lag - (cols - 1), first_lag + rows - 1
    lag = (
        first_lag
        + lax.broadcasted_iota(jnp.int32, (rows, cols), 0)
        - lax.broadcasted_iota(jnp.int32, (rows, cols), 1)
    )
    count = jnp.zeros((rows, cols), jnp.int32)
    for window, dilation in PATTERNS:
        if high < 0 or low > window:
            continue
        reads = (lag & (dilation - 1)) == 0
        if low < 0:
            reads = reads & (lag >= 0)
        if high > window:
            reads = reads & (lag <= window)
        count = count + reads.astype(jnp.int32)
    return jnp.where(
        count == 0,
        NEG,
        jnp.where(count == 1, 0.0, jnp.where(count == 2, 1.0, math.log2(3.0))),
    )


def kernel(
    n_grp,
    n_sp,
    n_tp,
    reach,
    tok_hbm,
    gain_ref,
    wq_hbm,
    wk_hbm,
    wv_hbm,
    og_hbm,
    wo_hbm,
    out_ref,
    tok,
    scaled,
    wq,
    wk,
    wv,
    og,
    wo,
    query,
    kv,
    guest,
    allowed,
    top,
    total,
    partial,
    help_att,
    help_lse,
    back_att,
    back_lse,
    att,
    got,
    load_sem,
    kv_send,
    kv_recv,
    q_send,
    q_recv,
    help_send,
    back_recv,
    wo_send,
    wo_recv,
    wo_fsend,
    wo_ysend,
    og_send,
    og_recv,
    att_send,
    att_recv,
):
    z = lax.axis_index("sp")
    me = lax.axis_index("tp")
    grp = lax.axis_index("grp")
    rows = query.shape[1]
    lanes = query.shape[2]
    channels = 2 * lanes
    heads = lanes // HEAD_DIM
    share = rows // n_tp
    chips = n_tp // 2
    chip, core = me // 2, lax.rem(me, 2)
    sibling = chip * 2 + 1 - core
    has_next = z + 1 < n_sp
    helped = n_sp == 4 and reach == 3
    paired = n_grp % 2 == 0
    far = grp + 1 - 2 * lax.rem(grp, 2) if paired else grp
    side = lax.rem(grp, 2) if paired else 0

    loads = [
        pltpu.make_async_copy(source, target, load_sem.at[number])
        for number, (source, target) in enumerate(
            ((tok_hbm, tok), (wk_hbm, wk), (wv_hbm, wv), (wq_hbm, wq), (og_hbm, og.at[me]), (wo_hbm, wo.at[me]))
        )
    ]
    for load in loads:
        load.start()

    barrier = pltpu.get_barrier_semaphore()
    for step in range(1, n_tp):
        pl.semaphore_signal(
            barrier, inc=1, device_id={"tp": lax.rem(me + step, n_tp)}, device_id_type=MESH
        )

    if paired:
        pl.semaphore_signal(barrier, inc=1, device_id={"grp": far}, device_id_type=MESH)
    for hop in ((1, 2) if helped else (1,)):
        if hop == 1:
            backward, onward = z > 0, has_next
        else:
            backward, onward = z == 3, z == 1

        @pl.when(backward)
        def _():
            pl.semaphore_signal(barrier, inc=1, device_id={"sp": z - hop}, device_id_type=MESH)

        @pl.when(onward)
        def _():
            pl.semaphore_signal(barrier, inc=1, device_id={"sp": z + hop}, device_id_type=MESH)

    def mark(distances):
        for distance in distances:
            for first in range(0, rows, ROW_BLOCK):
                allowed[distance, pl.ds(first, ROW_BLOCK), :] = log_multiplicity(
                    ROW_BLOCK, rows, first + distance * rows
                )

    mark(range(1))
    neighbours = (z > 0).astype(jnp.int32) + has_next.astype(jnp.int32)
    if helped:
        neighbours = neighbours + (z == 3).astype(jnp.int32) + (z == 1).astype(jnp.int32)
    pl.semaphore_wait(barrier, n_tp - 1 + int(paired) + neighbours)

    half = channels // PIECES
    own_pieces = PIECES // 2 if paired else PIECES

    def part_of(piece):
        return pl.ds(pl.multiple_of(piece * half, half), half)

    def wo_copy(slot, piece, target):
        return pltpu.make_async_remote_copy(
            src_ref=wo_hbm.at[part_of(piece)],
            dst_ref=wo.at[me, part_of(piece)],
            send_sem=wo_send.at[slot, piece],
            recv_sem=wo_recv.at[me, piece],
            device_id={"tp": target},
            device_id_type=MESH,
        )

    mine = [side * own_pieces + number for number in range(own_pieces)]
    theirs = [(1 - side) * own_pieces + number for number in range(own_pieces)] if paired else []
    across = [lax.rem(chip + step, chips) * 2 + core for step in range(1, chips)]
    wo_sends = [
        wo_copy(slot, piece, target) for piece in mine for slot, target in enumerate(across)
    ] + [wo_copy(chips - 1, piece, sibling) for piece in range(PIECES)]
    for copy in wo_sends:
        copy.start()

    def passed_on(shard, piece, send_sem, device):
        return pltpu.make_async_remote_copy(
            src_ref=wo.at[shard, part_of(piece)],
            dst_ref=wo.at[shard, part_of(piece)],
            send_sem=send_sem,
            recv_sem=wo_recv.at[shard, piece],
            device_id=device,
            device_id_type=MESH,
        )

    def wo_arrived(shard, piece):
        passed_on(shard, piece, wo_send.at[0, piece], {"tp": sibling}).wait_recv()

    forwards = []

    def forward(pieces, over_y):
        for piece in pieces:
            for step in range(1, chips):
                shard = across[step - 1]
                wo_arrived(shard, piece)
                copies = [passed_on(shard, piece, wo_fsend.at[step, piece], {"tp": sibling})]
                if over_y:
                    copies.insert(0, passed_on(shard, piece, wo_ysend.at[step, piece], {"grp": far}))
                for copy in copies:
                    copy.start()
                forwards.extend(copies)

    og_sends = [
        pltpu.make_async_remote_copy(
            src_ref=og_hbm,
            dst_ref=og.at[me],
            send_sem=og_send.at[step],
            recv_sem=og_recv.at[me],
            device_id={"tp": lax.rem(me + step, n_tp)},
            device_id_type=MESH,
        )
        for step in range(1, n_tp)
    ]
    for copy in og_sends:
        copy.start()

    def relay(part, distance):
        return pltpu.make_async_remote_copy(
            src_ref=kv.at[part, distance],
            dst_ref=kv.at[part, distance + 1],
            send_sem=kv_send.at[part, distance],
            recv_sem=kv_recv.at[part, distance + 1],
            device_id={"sp": z + 1},
            device_id_type=MESH,
        )

    def arrived(part, distance):
        pltpu.make_async_remote_copy(
            src_ref=kv.at[part, distance],
            dst_ref=kv.at[part, distance],
            send_sem=kv_send.at[part, 0],
            recv_sem=kv_recv.at[part, distance],
            device_id={"sp": z - 1},
            device_id_type=MESH,
        ).wait_recv()

    def ship(part, slot, target):
        return pltpu.make_async_remote_copy(
            src_ref=query.at[part],
            dst_ref=guest.at[slot],
            send_sem=q_send.at[part],
            recv_sem=q_recv.at[slot],
            device_id={"sp": target},
            device_id_type=MESH,
        )

    def guest_arrived(slot):
        ship(0, slot, z + 1).wait_recv()

    def send_back(slot, part, target):
        return [
            pltpu.make_async_remote_copy(
                src_ref=mine_ref.at[slot],
                dst_ref=their_ref.at[part],
                send_sem=help_send.at[slot, number],
                recv_sem=back_recv.at[part, number],
                device_id={"sp": target},
                device_id_type=MESH,
            )
            for number, (mine_ref, their_ref) in enumerate(((help_att, back_att), (help_lse, back_lse)))
        ]

    loads[0].wait()
    wide = tok[...].astype(jnp.float32)
    inverse = lax.rsqrt(jnp.mean(wide * wide, axis=-1, keepdims=True) + EPS)
    scaled[...] = (wide * gain_ref[...]).astype(jnp.bfloat16)

    def project(weight):
        product = jnp.dot(scaled[...], weight[...], preferred_element_type=jnp.float32)
        return (product * inverse).astype(jnp.bfloat16)

    def by_half(product):
        return product[:, :lanes], product[:, lanes:]

    loads[1].wait()
    kv[0, 0, 0], kv[1, 0, 0] = by_half(project(wk))
    loads[2].wait()
    kv[0, 0, 1], kv[1, 0, 1] = by_half(project(wv))

    @pl.when(has_next)
    def _():
        relay(0, 0).start()

    @pl.when(has_next & (z != 1) if helped else has_next)
    def _():
        relay(1, 0).start()

    loads[3].wait()
    query[0], query[1] = by_half(project(wq))
    if helped:

        @pl.when(z == 2)
        def _():
            ship(1, 0, 1).start()

        @pl.when(z == 3)
        def _():
            ship(1, 1, 1).start()
            ship(0, 1, 2).start()

    mark(range(1, reach + 1))
    lane_head = lax.broadcasted_iota(jnp.int32, (ROW_BLOCK, lanes), 1) // HEAD_DIM
    factor = HEAD_DIM ** (-0.5) * math.log2(math.e)

    def spread(columns):
        result = jnp.broadcast_to(columns[0], (ROW_BLOCK, lanes))
        for head in range(1, heads):
            result = jnp.where(
                lane_head == head, jnp.broadcast_to(columns[head], (ROW_BLOCK, lanes)), result
            )
        return result

    def stacked(rows_of):
        return jnp.concatenate(
            [jnp.where(lane_head == head, rows_of, jnp.zeros_like(rows_of)) for head in range(heads)],
            axis=0,
        )

    ones = jnp.ones((rows, lanes), jnp.bfloat16)

    def by_head(tall):
        result = tall[:ROW_BLOCK]
        for head in range(1, heads):
            result = jnp.where(
                lane_head == head, tall[head * ROW_BLOCK : (head + 1) * ROW_BLOCK], result
            )
        return result

    def attend(parts, state_of, queries_of, slot, distance, fresh):
        for part in parts:
            state = state_of(part)
            for first in range(0, rows, ROW_BLOCK):
                cols = min(rows, first + ROW_BLOCK) if distance == 0 else rows
                if first + distance * rows - (cols - 1) > REACH:
                    continue
                block = pl.ds(first, ROW_BLOCK)
                scores = lax.dot_general(
                    stacked(queries_of(part)[block, :]),
                    kv[part, slot, 0, :cols, :],
                    (((1,), (1,)), ((), ())),
                    preferred_element_type=jnp.float32,
                )
                bias = allowed[distance, block, :cols]
                scores = scores * factor + jnp.concatenate([bias] * heads, axis=0)
                peak = jnp.max(scores, axis=-1, keepdims=True)
                if not fresh:
                    old = jnp.concatenate([top[state, head, block, :] for head in range(heads)], axis=0)
                    peak = jnp.maximum(peak, old)
                    shrink = by_head(jnp.broadcast_to(jnp.exp2(old - peak), (heads * ROW_BLOCK, lanes)))
                for head in range(heads):
                    top[state, head, block, :] = peak[head * ROW_BLOCK : (head + 1) * ROW_BLOCK]
                weights = jnp.exp2(scores - peak).astype(jnp.bfloat16)
                extended = jnp.concatenate([kv[part, slot, 1, :cols, :], ones[:cols]], axis=1)
                product = jnp.dot(weights, extended, preferred_element_type=jnp.float32)
                mixed, sums = by_head(product[:, :lanes]), by_head(product[:, lanes:])
                if not fresh:
                    mixed = mixed + shrink * partial[state, block, :]
                    sums = sums + shrink * total[state, block, :]
                partial[state, block, :] = mixed
                total[state, block, :] = sums

    def own(parts, distance):
        attend(parts, lambda part: part, lambda part: query.at[part], distance, distance, distance == 0)

    def help_out(part, guest_slot, slot, distance, fresh):
        attend(
            [part], lambda _: 2 + guest_slot, lambda _: guest.at[guest_slot], slot, distance, fresh
        )

    def give_back(guest_slot, part, target):
        state = 2 + guest_slot
        lane = lax.broadcasted_iota(jnp.int32, (ROW_BLOCK, 128), 1)
        pick = (
            lax.broadcasted_iota(jnp.int32, (8, 128), 0) == lax.broadcasted_iota(jnp.int32, (8, 128), 1)
        ).astype(jnp.float32)
        for first in range(0, rows, ROW_BLOCK):
            block = pl.ds(first, ROW_BLOCK)
            sums = total[state, block, :]
            help_att[guest_slot, block, :] = (partial[state, block, :] / sums).astype(jnp.bfloat16)
            logs = jnp.zeros((ROW_BLOCK, 128), jnp.float32)
            for head in range(heads):
                column = top[state, head, block, :] + jnp.log2(sums[:, head * HEAD_DIM : head * HEAD_DIM + 1])
                logs = jnp.where(lane == head, jnp.broadcast_to(column, (ROW_BLOCK, 128)), logs)
            help_lse[guest_slot, :, block] = lax.dot_general(
                pick,
                logs,
                (((1,), (1,)), ((), ())),
                precision=lax.Precision.HIGHEST,
                preferred_element_type=jnp.float32,
            )
        for copy in send_back(guest_slot, part, target):
            copy.start()

    def take_back(part):
        for copy in send_back(0, part, z):
            copy.wait_recv()
        eye = (
            lax.broadcasted_iota(jnp.int32, (ROW_BLOCK, ROW_BLOCK), 0)
            == lax.broadcasted_iota(jnp.int32, (ROW_BLOCK, ROW_BLOCK), 1)
        ).astype(jnp.float32)
        for first in range(0, rows, ROW_BLOCK):
            block = pl.ds(first, ROW_BLOCK)
            logs = lax.dot_general(
                eye,
                back_lse[part, :, block],
                (((1,), (1,)), ((), ())),
                precision=lax.Precision.HIGHEST,
                preferred_element_type=jnp.float32,
            )
            before, after = [], []
            for head in range(heads):
                column, old = logs[:, head : head + 1], top[part, head, block, :]
                peak = jnp.maximum(column, old)
                before.append(jnp.exp2(old - peak))
                after.append(jnp.exp2(column - peak))
            wide_before, wide_after = spread(before), spread(after)
            total[part, block, :] = total[part, block, :] * wide_before + wide_after
            partial[part, block, :] = (
                partial[part, block, :] * wide_before
                + back_att[part, block, :].astype(jnp.float32) * wide_after
            )

    both = (0, 1)
    if helped:

        own(both, 0)
        early = own_pieces // 2
        forward(mine[:early], paired)

        @pl.when(z == 1)
        def _():
            arrived(0, 1)
            relay(0, 1).start()
            guest_arrived(1)
            help_out(1, 1, 0, 2, True)
            guest_arrived(0)
            help_out(1, 0, 0, 1, True)
            own([0], 1)

        @pl.when(z == 2)
        def _():
            arrived(0, 1)
            guest_arrived(1)
            help_out(0, 1, 1, 2, True)
            own([0], 1)

        @pl.when(z == 3)
        def _():
            arrived(0, 1)
            own([0], 1)

        forward(mine[early:], paired)

        @pl.when(z == 1)
        def _():
            arrived(1, 1)
            help_out(1, 1, 1, 3, False)
            give_back(1, 1, 3)
            help_out(1, 0, 1, 2, False)
            give_back(0, 1, 2)
            own([1], 1)

        @pl.when(z == 2)
        def _():
            arrived(0, 2)
            help_out(0, 1, 2, 3, False)
            give_back(1, 0, 3)
            own([0], 2)
            take_back(1)

        @pl.when(z == 3)
        def _():
            arrived(1, 1)
            own([1], 1)
            take_back(1)
            take_back(0)

    else:
        own(both, 0)
        for distance in range(1, reach + 1):

            @pl.when(z >= distance)
            def _():
                for part in both:
                    arrived(part, distance)
                    if distance < reach:

                        @pl.when(has_next)
                        def _():
                            relay(part, distance).start()

                own(both, distance)

        forward(mine, paired)

    def att_copy(step):
        target = lax.rem(me + step, n_tp)
        return pltpu.make_async_remote_copy(
            src_ref=att.at[target],
            dst_ref=got.at[me],
            send_sem=att_send.at[step],
            recv_sem=att_recv.at[me],
            device_id={"tp": target},
            device_id_type=MESH,
        )

    for target in range(n_tp):
        piece = pl.ds(target * share, share)
        for part in both:
            att[target, :, part * lanes : (part + 1) * lanes] = (
                partial[part, piece, :] / total[part, piece, :]
            ).astype(jnp.bfloat16)
    att_sends = [att_copy(step) for step in range(1, n_tp)]
    for copy in att_sends:
        copy.start()

    forward(theirs, False)
    loads[4].wait()
    loads[5].wait()
    for step in range(1, n_tp):
        peer = lax.rem(me + step, n_tp)
        pltpu.make_async_remote_copy(
            src_ref=og_hbm,
            dst_ref=og.at[peer],
            send_sem=og_send.at[step],
            recv_sem=og_recv.at[peer],
            device_id={"tp": peer},
            device_id_type=MESH,
        ).wait_recv()
    for piece in range(PIECES):
        wo_arrived(sibling, piece)
        for step in range(1, chips):
            wo_arrived(lax.rem(chip + step, chips) * 2 + 1 - core, piece)

    def norm_and_gate(rows_of, gain_of):
        row_values = rows_of.astype(jnp.float32)
        return (
            jnp.sum(row_values * row_values, axis=-1, keepdims=True),
            (row_values * gain_of).astype(jnp.bfloat16),
        )

    squares, gated = norm_and_gate(att[me], og[me])
    summed = jnp.dot(gated, wo[me], preferred_element_type=jnp.float32)
    for step in range(1, n_tp):
        peer = lax.rem(me + step, n_tp)
        pltpu.make_async_remote_copy(
            src_ref=att.at[peer],
            dst_ref=got.at[peer],
            send_sem=att_send.at[step],
            recv_sem=att_recv.at[peer],
            device_id={"tp": peer},
            device_id_type=MESH,
        ).wait_recv()
        more, gated = norm_and_gate(got[peer], og[peer])
        squares = squares + more
        summed = summed + jnp.dot(gated, wo[peer], preferred_element_type=jnp.float32)
    norm = lax.rsqrt(squares / (channels * n_tp) + EPS)
    out_ref[...] = (summed * norm).astype(jnp.bfloat16)

    for copy in wo_sends + og_sends + att_sends + forwards:
        copy.wait_send()
    if helped:

        @pl.when(z == 1)
        def _():
            relay(0, 0).wait_send()
            relay(0, 1).wait_send()
            for copy in send_back(1, 1, 3) + send_back(0, 1, 2):
                copy.wait_send()

        @pl.when((z == 0) | (z == 2))
        def _():
            relay(0, 0).wait_send()
            relay(1, 0).wait_send()

        @pl.when(z == 2)
        def _():
            ship(1, 0, 1).wait_send()
            for copy in send_back(1, 0, 3):
                copy.wait_send()

        @pl.when(z == 3)
        def _():
            ship(1, 1, 1).wait_send()
            ship(0, 1, 2).wait_send()

    else:
        for distance in range(reach):

            @pl.when(has_next & (z >= distance))
            def _():
                for part in both:
                    relay(part, distance).wait_send()


def on_device(n_grp, n_sp, n_tp, tokens, norm_gain, w_query, w_key, w_value, out_gain, w_out):
    rows, width = tokens.shape
    channels = w_query.shape[1]
    lanes = channels // 2
    heads = lanes // HEAD_DIM
    share = rows // n_tp
    reach = min(-(-REACH // rows), n_sp - 1)
    hbm = pl.BlockSpec(memory_space=pl.ANY)
    vmem = pl.BlockSpec(memory_space=pltpu.VMEM)
    dma = pltpu.SemaphoreType.DMA
    bf16, f32 = jnp.bfloat16, jnp.float32
    return pl.pallas_call(
        functools.partial(kernel, n_grp, n_sp, n_tp, reach),
        out_shape=jax.ShapeDtypeStruct((share, w_out.shape[1]), bf16),
        in_specs=[hbm, vmem, hbm, hbm, hbm, hbm, hbm],
        out_specs=vmem,
        scratch_shapes=[
            pltpu.VMEM((rows, width), bf16),
            pltpu.VMEM((rows, width), bf16),
            pltpu.VMEM((width, channels), bf16),
            pltpu.VMEM((width, channels), bf16),
            pltpu.VMEM((width, channels), bf16),
            pltpu.VMEM((n_tp, 1, channels), f32),
            pltpu.VMEM((n_tp,) + w_out.shape, bf16),
            pltpu.VMEM((2, rows, lanes), bf16),
            pltpu.VMEM((2, reach + 1, 2, rows, lanes), bf16),
            pltpu.VMEM((2, rows, lanes), bf16),
            pltpu.VMEM((reach + 1, rows, rows), f32),
            pltpu.VMEM((4, heads, rows, 1), f32),
            pltpu.VMEM((4, rows, lanes), f32),
            pltpu.VMEM((4, rows, lanes), f32),
            pltpu.VMEM((2, rows, lanes), bf16),
            pltpu.VMEM((2, 8, rows), f32),
            pltpu.VMEM((2, rows, lanes), bf16),
            pltpu.VMEM((2, 8, rows), f32),
            pltpu.VMEM((n_tp, share, channels), bf16),
            pltpu.VMEM((n_tp, share, channels), bf16),
            dma((6,)),
            dma((2, reach + 1)),
            dma((2, reach + 1)),
            dma((2,)),
            dma((2,)),
            dma((2, 2)),
            dma((2, 2)),
            dma((n_tp // 2, PIECES)),
            dma((n_tp, PIECES)),
            dma((n_tp // 2, PIECES)),
            dma((n_tp // 2, PIECES)),
            dma((n_tp,)),
            dma((n_tp,)),
            dma((n_tp,)),
            dma((n_tp,)),
        ],
        compiler_params=pltpu.CompilerParams(
            collective_id=0, has_side_effects=True, vmem_limit_bytes=60 * 1024 * 1024
        ),
    )(tokens, norm_gain[None, :], w_query, w_key, w_value, out_gain[None, :], w_out)


def solution(mesh):
    in_specs = (
        P(("grp", "sp"), None),
        P(),
        P(None, "tp"),
        P(None, "tp"),
        P(None, "tp"),
        P("tp"),
        P("tp", None),
    )
    out_specs = P(("grp", "sp", "tp"), None)
    return jax.shard_map(
        functools.partial(on_device, mesh.shape["grp"], mesh.shape["sp"], mesh.shape["tp"]),
        mesh=mesh,
        in_specs=in_specs,
        out_specs=out_specs,
        check_vma=False,
    )
```
